32 devices in a mesh: sp: 8 (over z, core), tp: 4 (over y, x).
Axes of the slice: x: 2, y: 2, z: 4, core: 2. Of those that a mesh axis runs over, the one named last changes fastest.
Arguments:
- residual: bfloat16 [3072, 4096], P('sp', 'tp'), may hold values from -10 to 10
- query_nope: bfloat16 [3072, 1024], P('sp', 'tp'), may hold values from -6 to 6
- query_rope: bfloat16 [3072, 512], P('sp', 'tp'), may hold values from -10 to 10
- latent: bfloat16 [3072, 512], P('sp'), may hold values from -8 to 8
- key_rope: bfloat16 [3072, 32], P('sp'), may hold values from -10 to 10
- latent_gain: float32 [512], replicated, may hold values from 0.1 to 1.9
- key_up: bfloat16 [512, 1024], P(None, 'tp'), may hold values from -0.25 to 0.25
- value_up: bfloat16 [512, 1024], P(None, 'tp'), may hold values from -0.25 to 0.25
- out_proj: bfloat16 [1024, 4096], P(None, 'tp'), may hold values from -0.625 to 0.625
- norm_gain: float32 [4096], P('tp'), may hold values from 0.1 to 1.9
- routes: int32 [3072, 2], P('sp'), may hold values from 0 to 7, all different within a row; in each aligned block of 384 rows (0 to 383, 384 to 767, ...) at most 120 rows name the same one
- route_weight: float32 [3072, 2], P('sp'), may hold values from 0.2 to 1
- expert_gate: bfloat16 [8, 4096, 1024], P('sp', None, 'tp'), may hold values from -0.09375 to 0.09375
- expert_up: bfloat16 [8, 4096, 1024], P('sp', None, 'tp'), may hold values from -0.09375 to 0.09375
- expert_down: bfloat16 [8, 1024, 4096], P('sp', None, 'tp'), may hold values from -0.1875 to 0.1875
Outputs:
- mixed_out: bfloat16 [3072, 4096], P('sp', 'tp')
The draws below stay inside these ranges and needn't reach their ends.
Inputs may be any that keep to these rules, and one draw needn't show every extreme that they name: `routes`: each row names 2 different experts. In each aligned block of 384 rows no expert is named more than 120 times, and in some blocks one expert is named exactly 120 times.
All inputs are finite; a program needn't handle non-finite values.
Results may differ from the reference program's by a relative error of at most 0.01.
Values may be sent and summed in bfloat16 or wider, within the bound.
A program may use at most 64 MiB of HBM per device.

```python
import math
import jax
import jax.numpy as jnp
import numpy as np
from jax import lax

MODEL_DIM = 4096
HEAD_COUNT = 16
NOPE_DIM = 64
ROPE_DIM = 32
VALUE_DIM = 64
KV_RANK = 512
FF_DIM = 1024
TOP_K = 2
TOK_SP = 384
SEQ_LEN = 3072
EXPERTS = 8
CAPACITY = 120


def rope_pair(base_key):
    key_one, key_two = jax.random.split(base_key, 2)
    key_vals = jnp.clip(jax.random.normal(key_one, (SEQ_LEN, ROPE_DIM), jnp.float32), -5.0, 5.0)
    query_vals = jnp.clip(jax.random.normal(key_two, (SEQ_LEN, HEAD_COUNT, ROPE_DIM), jnp.float32), -5.0, 5.0)
    return (query_vals.reshape(SEQ_LEN, HEAD_COUNT * ROPE_DIM), key_vals)


def draw_query_rope(key, part):
    return rope_pair(jax.random.fold_in(key, 17))[0].astype(jnp.bfloat16)


def draw_key_rope(key, part):
    return rope_pair(jax.random.fold_in(key, 17))[1].astype(jnp.bfloat16)


def draw_latent(key, part):
    key_noise, key_mean = jax.random.split(key)
    regions = (SEQ_LEN + 255) // 256
    region_means = 0.8 * jax.random.normal(key_mean, (regions, KV_RANK), jnp.float32)
    noise_vals = jax.random.normal(key_noise, (SEQ_LEN, KV_RANK), jnp.float32)
    region_index = jnp.arange(SEQ_LEN) // 256
    return jnp.clip(noise_vals + region_means[region_index], -8.0, 8.0).astype(jnp.bfloat16)


def draw_residual(key, part):
    key_vals, key_phase, key_rough = jax.random.split(key, 3)
    columns = jnp.arange(MODEL_DIM, dtype=jnp.float32) / MODEL_DIM
    phase_shift = jax.random.uniform(key_phase, (), jnp.float32, 0.0, 6.2831853)
    rough_factor = jax.random.uniform(key_rough, (MODEL_DIM,), jnp.float32, 0.7, 1.3)
    column_scale = jnp.exp(1.1 * jnp.cos(6.2831853 * 3.0 * columns + phase_shift)) * rough_factor
    noise_vals = jax.random.normal(key_vals, (SEQ_LEN, MODEL_DIM), jnp.float32)
    return jnp.clip(noise_vals * column_scale[None, :], -10.0, 10.0).astype(jnp.bfloat16)


def levels(rng, extent, cuts, low, largest):
    def one(position, blocks):
        steps = jax.random.uniform(jax.random.fold_in(jax.random.fold_in(rng, 6), position), (blocks,), jnp.float32, low / len(cuts), largest / len(cuts))
        return jnp.repeat(jnp.exp(steps), extent[position] // blocks).reshape((-1,) + (1,) * (len(extent) - position - 1))

    gain = one(*cuts[0])
    for cut in cuts[1:]:
        gain = gain * one(*cut)
    return gain


def routed_block(own_key, own, number, rows, count, top, bound, slope):
    sequence = jax.random.permutation(own_key, count)
    crowded, common = shares(count, rows * top, bound, slope, True), shares(count, rows * top, bound, slope, False)
    places = jnp.arange(count)

    def named(sizes, turn):
        used = int((sizes > 0).sum())
        fixed = max(1, used // 4)
        shifted = fixed + (places - fixed + turn * (used - fixed)) % max(1, count - fixed)
        return jnp.zeros((count,), jnp.int32).at[sequence[jnp.where(places < fixed, places, shifted)]].set(jnp.asarray(sizes, jnp.int32))

    sizes = jnp.where(number % 4 == 0, named(crowded, number // 4), named(common, number - number // 4 - 1))
    mixed = jax.random.permutation(jax.random.fold_in(own, 3), count)
    donor, receiver = mixed[0:count // 2 * 2:2], mixed[1:count // 2 * 2:2]
    margin = jnp.minimum(sizes[donor] - 1, bound - sizes[receiver]) // 2
    margin = jnp.where((donor == sequence[0]) | (receiver == sequence[0]) | (sizes[receiver] == 0), 0, jnp.maximum(margin, 0))
    shifted = jax.random.randint(jax.random.fold_in(own, 4), (count // 2,), 0, 1 << 20) % (margin + 1)
    sizes = sizes.at[donor].add(-shifted).at[receiver].add(shifted)
    members = jnp.searchsorted(jnp.cumsum(sizes), jnp.arange(rows * top), side="right").astype(jnp.int32)
    table = members.reshape(top, rows).T
    table = table[jax.random.permutation(jax.random.fold_in(own, 1), rows)]
    turn = jax.random.randint(jax.random.fold_in(own, 2), (rows, 1), 0, top)
    return jnp.take_along_axis(table, (jnp.arange(top)[None, :] + turn) % top, axis=1)


def shares(amount, total, bound, slope, full):
    portions = [(1 << 20) // math.isqrt(grade ** slope) + 1 for grade in range(1, amount + 1)]
    largest = bound if full else min(bound, max(-(-total // amount), total * portions[0] // sum(portions)))
    least = 1 if total - largest >= amount - 1 else 0
    given, rest = [largest] + [least] * (amount - 1), total - largest - least * (amount - 1)
    while rest > 0:
        free = [i for i in range(1, amount) if given[i] < largest] or [i for i in range(1, amount) if given[i] < bound]
        whole, remaining = sum([portions[i] for i in free]), rest
        for i in free:
            more = min(bound - given[i], max(1, remaining * portions[i] // whole), rest)
            given[i] = given[i] + more
            rest = rest - more
    return np.array(given)


def gaussian(rng, dims, spread, most, cuts=(), kind=jnp.bfloat16):
    loudness = levels(rng, dims, cuts, -0.22, 0.18) if cuts else 1.0
    values = jax.random.normal(rng, dims, jnp.float32) * spread * loudness
    return jnp.minimum(jnp.maximum(values, -most), most).astype(kind)


def setup_inputs(seed: int = 0) -> dict:
    key_list = jax.random.split(jax.random.key(seed), 16)
    residual = draw_residual(jax.random.fold_in(key_list[15], 71), 0)
    query_nope = gaussian(key_list[1], (SEQ_LEN, HEAD_COUNT * NOPE_DIM), 1.0, 6.0, ((0, 8), (1, 4)))
    query_rope = draw_query_rope(jax.random.fold_in(key_list[15], 71), 0)
    latent = draw_latent(jax.random.fold_in(key_list[15], 71), 0)
    key_rope = draw_key_rope(jax.random.fold_in(key_list[15], 71), 0)
    latent_gain = jnp.clip(1.0 + 0.18 * jax.random.normal(key_list[5], (KV_RANK,), jnp.float32), 0.1, 1.9)
    key_up = gaussian(key_list[6], (KV_RANK, HEAD_COUNT * NOPE_DIM), KV_RANK ** -0.5, 0.25, ((1, 4),))
    value_up = gaussian(key_list[7], (KV_RANK, HEAD_COUNT * VALUE_DIM), KV_RANK ** -0.5, 0.25, ((1, 4),))
    out_proj = gaussian(key_list[8], (HEAD_COUNT * VALUE_DIM, MODEL_DIM), 0.1, 0.625, ((1, 4),))
    norm_gain = jnp.clip(1.0 + 0.18 * jax.random.normal(key_list[9], (MODEL_DIM,), jnp.float32), 0.1, 1.9)
    routes_keys = jax.random.split(jax.random.fold_in(key_list[10], 1), SEQ_LEN // TOK_SP)
    routes_turns = jax.random.permutation(jax.random.fold_in(key_list[10], 3), SEQ_LEN // TOK_SP)
    routes = jax.vmap(lambda own, number: routed_block(jax.random.fold_in(key_list[10], 2), own, number, TOK_SP, EXPERTS, TOP_K, CAPACITY, 1))(routes_keys, routes_turns).reshape((SEQ_LEN, TOP_K))
    route_weight = jnp.clip(0.2 + 0.8 * jax.random.uniform(key_list[11], (SEQ_LEN, TOP_K), jnp.float32) ** levels(key_list[11], (SEQ_LEN, TOP_K), ((0, 8),), -0.2, 0.2), 0.2, 1.0)
    expert_gate = gaussian(key_list[12], (EXPERTS, MODEL_DIM, FF_DIM), MODEL_DIM ** -0.5, 0.09375, ((0, 8), (2, 4)))
    expert_up = gaussian(key_list[13], (EXPERTS, MODEL_DIM, FF_DIM), MODEL_DIM ** -0.5, 0.09375, ((0, 8), (2, 4)))
    expert_down = gaussian(key_list[14], (EXPERTS, FF_DIM, MODEL_DIM), FF_DIM ** -0.5, 0.1875, ((0, 8), (2, 4)))
    return {"residual": residual, "query_nope": query_nope, "query_rope": query_rope, "latent": latent, "key_rope": key_rope, "latent_gain": latent_gain, "key_up": key_up, "value_up": value_up, "out_proj": out_proj, "norm_gain": norm_gain, "routes": routes, "route_weight": route_weight, "expert_gate": expert_gate, "expert_up": expert_up, "expert_down": expert_down}


epsilon = 1e-06
rope_base = 10000.0
negative = -1e+30

def widen_back(values_in):
    return lax.optimization_barrier(values_in).astype(jnp.float32)

def rotate(values_in, places):
    half_dim = values_in.shape[-1] // 2
    inverse = rope_base ** (-jnp.arange(half_dim, dtype=jnp.float32) / half_dim)
    angles = places.astype(jnp.float32)[:, None] * inverse[None, :]
    angles = angles.reshape((angles.shape[0],) + (1,) * (values_in.ndim - 2) + (half_dim,))
    cosine = jnp.cos(angles)
    sine_wave = jnp.sin(angles)
    first_half = values_in[..., :half_dim]
    second_half = values_in[..., half_dim:]
    return jnp.concatenate([first_half * cosine - second_half * sine_wave, first_half * sine_wave + second_half * cosine], axis=-1)

def norm_rows(values_in, gain_vec):
    wide = values_in.astype(jnp.float32)
    mean_square = lax.optimization_barrier(jnp.mean(wide * wide, axis=-1, keepdims=True))
    return (wide * lax.rsqrt(mean_square + epsilon) * gain_vec[None, :]).astype(jnp.bfloat16)

def reference(residual, query_nope, query_rope, latent, key_rope, latent_gain, key_up, value_up, out_proj, norm_gain, routes, route_weight, expert_gate, expert_up, expert_down):
    seq_rows = residual.shape[0]
    head_total = query_nope.shape[1] // NOPE_DIM
    places = jnp.arange(seq_rows, dtype=jnp.int32)
    rot_query = rotate(query_rope.astype(jnp.float32).reshape(seq_rows, head_total, ROPE_DIM), places).astype(jnp.bfloat16)
    rot_key = rotate(key_rope.astype(jnp.float32), places).astype(jnp.bfloat16)
    latent_norm = norm_rows(latent, latent_gain)
    key_heads = jnp.dot(latent_norm, key_up, preferred_element_type=jnp.float32).astype(jnp.bfloat16)
    value_heads = jnp.dot(latent_norm, value_up, preferred_element_type=jnp.float32).astype(jnp.bfloat16)
    key_wide = widen_back(key_heads).reshape(seq_rows, head_total, NOPE_DIM)
    value_wide = widen_back(value_heads).reshape(seq_rows, head_total, VALUE_DIM)
    rope_wide = widen_back(rot_key)
    query_wide = query_nope.astype(jnp.float32).reshape(seq_rows, head_total, NOPE_DIM)
    rotq_wide = widen_back(rot_query)
    score_scale = (NOPE_DIM + ROPE_DIM) ** (-0.5)

    def attend(first_row):
        query_block = lax.dynamic_slice_in_dim(query_wide, first_row, TOK_SP, 0)
        rotary_block = lax.dynamic_slice_in_dim(rotq_wide, first_row, TOK_SP, 0)
        scores = (jnp.einsum('thd,shd->ths', query_block, key_wide) + jnp.einsum('thr,sr->ths', rotary_block, rope_wide)) * score_scale
        row_places = first_row + jnp.arange(TOK_SP, dtype=jnp.int32)
        allowed = (places[None, :] <= row_places[:, None])[:, None, :]
        scores = jnp.where(allowed, scores, negative)
        top_score = lax.optimization_barrier(jnp.max(scores, axis=-1, keepdims=True))
        weights = jnp.where(allowed, jnp.exp(scores - top_score), 0.0)
        denominator = lax.optimization_barrier(jnp.sum(weights, axis=-1))
        weight_b = widen_back(weights.astype(jnp.bfloat16))
        mixed_block = jnp.einsum('ths,shd->thd', weight_b, value_wide)
        return (mixed_block / denominator[:, :, None]).astype(jnp.bfloat16)
    starts = jnp.arange(seq_rows // TOK_SP, dtype=jnp.int32) * TOK_SP
    attended = lax.map(attend, starts).reshape(seq_rows, head_total * VALUE_DIM)
    projected = jnp.dot(attended, out_proj, preferred_element_type=jnp.float32)
    mid = (residual.astype(jnp.float32) + projected).astype(jnp.bfloat16)
    normed = norm_rows(mid, norm_gain)
    blocks = seq_rows // TOK_SP
    experts = expert_gate.shape[0]
    capacity = 5 * TOK_SP * TOP_K // (4 * experts)
    flat_routes = routes.reshape(blocks, TOK_SP * TOP_K).astype(jnp.int32)
    choose = (flat_routes[:, :, None] == jnp.arange(experts, dtype=jnp.int32)[None, None, :]).astype(jnp.int32)
    number = lax.optimization_barrier(jnp.sum((jnp.cumsum(choose, axis=1) - 1) * choose, axis=2)).astype(jnp.int32)
    block_index = jnp.broadcast_to(jnp.arange(blocks, dtype=jnp.int32)[:, None], flat_routes.shape)
    source = block_index * TOK_SP + jnp.arange(TOK_SP * TOP_K, dtype=jnp.int32)[None, :] // TOP_K
    slot_table = jnp.full((experts, blocks, capacity), seq_rows, jnp.int32).at[flat_routes, block_index, number].set(source)
    padded = jnp.concatenate([normed, jnp.zeros((1, normed.shape[1]), jnp.bfloat16)], axis=0)

    def serve_rows(expert):
        chosen = padded[slot_table[expert].reshape(-1)]
        gate_pre = jnp.dot(chosen, expert_gate[expert], preferred_element_type=jnp.float32)
        up_pre = jnp.dot(chosen, expert_up[expert], preferred_element_type=jnp.float32)
        hidden = (jax.nn.silu(gate_pre) * up_pre).astype(jnp.bfloat16)
        return jnp.dot(hidden, expert_down[expert], preferred_element_type=jnp.float32).astype(jnp.bfloat16)
    results = lax.map(serve_rows, jnp.arange(experts, dtype=jnp.int32))
    results = results.reshape(experts, blocks, capacity, results.shape[-1])
    picked = widen_back(results[flat_routes, block_index, number]).reshape(seq_rows, TOP_K, -1)
    routed_sum = lax.optimization_barrier(jnp.sum(picked * route_weight[:, :, None], axis=1))
    return (mid.astype(jnp.float32) + routed_sum).astype(jnp.bfloat16)
```

```python
import functools

import jax
import jax.numpy as jnp
from jax import lax
from jax.experimental import pallas as pl
from jax.experimental.pallas import tpu as pltpu
from jax.sharding import PartitionSpec as P

NOPE_DIM = 64
ROPE_DIM = 32
VALUE_DIM = 64
TOP_K = 2
LANES = 128

epsilon = 1e-06
rope_base = 10000.0
negative = -1e30
MESH = pl.DeviceIdType.MESH
bf16 = jnp.bfloat16
f32 = jnp.float32


def rotate(values_in, places):
    half_dim = values_in.shape[-1] // 2
    inverse = rope_base ** (-jnp.arange(half_dim, dtype=jnp.float32) / half_dim)
    angles = places.astype(jnp.float32)[:, None] * inverse[None, :]
    angles = angles.reshape((angles.shape[0],) + (1,) * (values_in.ndim - 2) + (half_dim,))
    cosine = jnp.cos(angles)
    sine_wave = jnp.sin(angles)
    first_half = values_in[..., :half_dim]
    second_half = values_in[..., half_dim:]
    return jnp.concatenate(
        [
            first_half * cosine - second_half * sine_wave,
            first_half * sine_wave + second_half * cosine,
        ],
        axis=-1,
    )


def norm_rows(values_in, gain_vec):
    wide = values_in.astype(jnp.float32)
    mean_square = jnp.mean(wide * wide, axis=-1, keepdims=True)
    return (wide * lax.rsqrt(mean_square + epsilon) * gain_vec[None, :]).astype(jnp.bfloat16)


def flip(a, b, n):
    total = 0
    bit = 1
    while bit < n:
        total = total + ((a // bit) % 2 + (b // bit) % 2) % 2 * bit
        bit *= 2
    return total


def attend_kernel(heads, q_ref, lat_ref, wk_ref, wv_ref, out_ref, top_ref, acc_ref):
    rows = q_ref.shape[0]
    me = lax.axis_index("sp")
    scale = (NOPE_DIM + ROPE_DIM) ** (-0.5) * 1.4426950408889634
    top_ref[...] = jnp.full(top_ref.shape, negative, f32)
    acc_ref[...] = jnp.zeros(acc_ref.shape, f32)

    def block(b, masked):
        lat = lat_ref[pl.ds(pl.multiple_of(b * rows, rows), rows), :]
        keys = jnp.dot(lat, wk_ref[...], preferred_element_type=f32).astype(bf16)
        values = jnp.dot(lat, wv_ref[...], preferred_element_type=f32).astype(bf16)
        for h in range(heads):
            cols = slice(h * LANES, (h + 1) * LANES)
            scores = lax.dot_general(
                q_ref[:, cols], keys[:, cols], (((1,), (1,)), ((), ())), preferred_element_type=f32
            )
            if masked:
                allowed = lax.broadcasted_iota(jnp.int32, scores.shape, 1) <= (
                    lax.broadcasted_iota(jnp.int32, scores.shape, 0)
                )
                scores = jnp.where(allowed, scores, negative)
            old = top_ref[h]
            new = jnp.maximum(old, jnp.max(scores, axis=1, keepdims=True))
            weights = jnp.exp2((scores - new[:, :1]) * scale)
            fading = jnp.exp2((old - new) * scale)
            top_ref[h] = new
            acc_ref[h] = acc_ref[h] * fading + jnp.dot(
                weights.astype(bf16), values[:, cols], preferred_element_type=f32
            )

    @pl.loop(0, me)
    def _(b):
        block(b, False)

    block(me, True)
    outs = []
    for h in range(heads):
        acc = acc_ref[h]
        outs.append(acc[:, :VALUE_DIM] / acc[:, VALUE_DIM : VALUE_DIM + 1])
    out_ref[...] = jnp.concatenate(outs, axis=1).astype(bf16)


def expert_kernel(
    S, T, C, M,
    att_ref, res_ref, wo_ref, gain_ref, slot_ref, cols_ref, *rest,
):
    w_hbm = rest[:T]
    down_hbm = rest[T]
    out_ref = rest[T + 1]
    (
        att_all, sq_own, sq_all, mid_ref, acc_ref, norm_ref, send, recv, psend, precv, own, hid, res, ret,
        w_ref, down_ref,
        load_sem, att_s, att_r, sq_s, sq_r, d_s, d_r, p_s, p_r, h_s, h_r, r_s, r_r,
    ) = rest[T + 2 :]
    me_s = lax.axis_index("sp")
    me_t = lax.axis_index("tp")
    rows, K = res_ref.shape
    heads_w = att_ref.shape[1]
    F = w_ref.shape[2] // 2

    loads = [pltpu.make_async_copy(w_hbm[d], w_ref.at[d], load_sem.at[d]) for d in range(T)]
    loads.append(pltpu.make_async_copy(down_hbm, down_ref, load_sem.at[T]))

    barrier = pltpu.get_barrier_semaphore()
    for d in range(1, T):
        pl.semaphore_signal(barrier, inc=1, device_id=(me_s, flip(me_t, d, T)), device_id_type=MESH)
    for j in range(1, S):
        pl.semaphore_signal(barrier, inc=1, device_id=(flip(me_s, j, S), me_t), device_id_type=MESH)
    pl.semaphore_wait(barrier, S + T - 2)

    def remote(src, dst, ss, rs, s, t):
        return pltpu.make_async_remote_copy(
            src_ref=src, dst_ref=dst, send_sem=ss, recv_sem=rs, device_id=(s, t), device_id_type=MESH
        )

    def att_copy(d):
        return remote(att_ref, att_all.at[d - 1], att_s.at[d - 1], att_r.at[d - 1], me_s, flip(me_t, d, T))

    def sq_copy(d):
        return remote(sq_own, sq_all.at[d - 1], sq_s.at[d - 1], sq_r.at[d - 1], me_s, flip(me_t, d, T))

    def d_copy(j):
        return remote(send.at[j], recv.at[j], d_s.at[j], d_r.at[j], flip(me_s, j, S), me_t)

    def p_copy(j, d):
        return remote(
            psend.at[j, d - 1], precv.at[j, d - 1], p_s.at[j % M, d - 1], p_r.at[j % M, d - 1],
            me_s, flip(me_t, d, T),
        )

    def h_copy(j, d):
        return remote(
            hid.at[j, 0], hid.at[j, d], h_s.at[j % M, d - 1], h_r.at[j % M, d - 1], me_s, flip(me_t, d, T)
        )

    def r_copy(j):
        return remote(res.at[j], ret.at[j], r_s.at[j], r_r.at[j], flip(me_s, j, S), me_t)

    for d in range(1, T):
        att_copy(d).start()
    for load in loads:
        load.start()

    def project(att, d):
        begin = pl.multiple_of(flip(me_t, d, T) * heads_w, heads_w)
        return jnp.dot(att, wo_ref[pl.ds(begin, heads_w), :], preferred_element_type=f32)

    acc_ref[...] = res_ref[...].astype(f32) + project(att_ref[...], 0)
    for d in range(1, T):
        att_copy(d).wait_recv()
        acc_ref[...] += project(att_all[d - 1], d)
    mid_ref[...] = acc_ref[...].astype(bf16)
    wide = mid_ref[...].astype(f32)
    square = jnp.sum(wide * wide, axis=1, keepdims=True)
    sq_own[...] = jnp.transpose(jnp.broadcast_to(square, (rows, LANES)))[:8]
    for d in range(1, T):
        sq_copy(d).start()
    total = sq_own[...]
    for d in range(1, T):
        sq_copy(d).wait_recv()
        total = total + sq_all[d - 1]
    row_scale = lax.rsqrt(total / (K * T) + epsilon)
    row_scale = jnp.transpose(jnp.broadcast_to(row_scale[:1], (LANES, rows)))[:, :1]
    wide = mid_ref[...].astype(f32)
    norm_ref[...] = (wide * row_scale * gain_ref[...]).astype(bf16)
    acc_ref[...] = wide

    def rows_for(j):
        base = (flip(me_s, j, S) * C).astype(f32)
        places = lax.broadcasted_iota(jnp.int32, (C, rows), 0).astype(f32) + base
        hit = (places == slot_ref[0:1, :]) | (places == slot_ref[1:2, :])
        picks = jnp.where(hit, 1.0, 0.0).astype(bf16)
        return jnp.dot(picks, norm_ref[...], preferred_element_type=f32).astype(bf16)

    @pl.loop(1, S)
    def _(j):
        send[j] = rows_for(j)
        d_copy(j).start()

    recv[0] = rows_for(0)
    for load in loads:
        load.wait()

    def add_result(j):
        base = (flip(me_s, j, S) * C).astype(f32)
        places = lax.broadcasted_iota(jnp.int32, (rows, C), 1).astype(f32) + base
        hit0 = places == cols_ref[:, 0:1]
        hit1 = places == cols_ref[:, 1:2]
        picks = jnp.where(hit0 | hit1, 1.0, 0.0).astype(bf16)
        inside0 = (cols_ref[:, 0:1] >= base) & (cols_ref[:, 0:1] < base + C)
        inside1 = (cols_ref[:, 1:2] >= base) & (cols_ref[:, 1:2] < base + C)
        share = jnp.where(inside0, cols_ref[:, 2:3], jnp.where(inside1, cols_ref[:, 3:4], 0.0))
        acc_ref[...] += share * jnp.dot(picks, ret[j], preferred_element_type=f32)

    @pl.loop(0, S + 2)
    def _(i):
        @pl.when(i < S)
        def _():
            j = i

            @pl.when(j > 0)
            def _():
                d_copy(j).wait_recv()

            block = recv[j]
            for d in range(1, T):
                if S > M:

                    @pl.when(j >= M)
                    def _():
                        p_copy(j - M, d).wait_send()

                psend[j, d - 1] = jnp.dot(block, w_ref[d], preferred_element_type=f32).astype(bf16)
                p_copy(j, d).start()
            own[j % 2] = jnp.dot(block, w_ref[0], preferred_element_type=f32)

        @pl.when((i >= 1) & (i < S + 1))
        def _():
            j = i - 1
            total = own[j % 2]
            for d in range(1, T):
                p_copy(j, d).wait_recv()
                total = total + precv[j, d - 1].astype(f32)
            gate = total[:, :F]
            hid[j, 0] = (gate / (1.0 + jnp.exp(-gate)) * total[:, F:]).astype(bf16)
            for d in range(1, T):
                if S > M:

                    @pl.when(j >= M)
                    def _():
                        h_copy(j - M, d).wait_send()

                h_copy(j, d).start()

        @pl.when(i >= 2)
        def _():
            j = i - 2
            total = jnp.zeros((C, K), f32)
            for d in range(T):
                if d > 0:
                    h_copy(j, d).wait_recv()
                begin = pl.multiple_of(flip(me_t, d, T) * F, F)
                total += jnp.dot(hid[j, d], down_ref[pl.ds(begin, F), :], preferred_element_type=f32)

            @pl.when(j > 0)
            def _():
                res[j] = total.astype(bf16)
                r_copy(j).start()

            @pl.when(j == 0)
            def _():
                ret[j] = total.astype(bf16)

    add_result(0)

    @pl.loop(1, S)
    def _(j):
        r_copy(j).wait_recv()
        add_result(j)

    out_ref[...] = acc_ref[...].astype(bf16)

    for d in range(1, T):
        att_copy(d).wait_send()
        sq_copy(d).wait_send()

    @pl.loop(S - M, S)
    def _(j):
        for d in range(1, T):
            p_copy(j, d).wait_send()
            h_copy(j, d).wait_send()

    @pl.loop(1, S)
    def _(j):
        d_copy(j).wait_send()
        r_copy(j).wait_send()


def per_device(
    residual, query_nope, query_rope, latent, key_rope, latent_gain, key_up, value_up, out_proj,
    norm_gain, routes, route_weight, expert_gate, expert_up, expert_down,
):
    rows, K = residual.shape
    S = lax.axis_size("sp")
    T = lax.axis_size("tp")
    me_s = lax.axis_index("sp")
    me_t = lax.axis_index("tp")
    heads = query_nope.shape[1] // NOPE_DIM
    rank = latent.shape[1]
    F = expert_gate.shape[2]

    width = -(-(rank + ROPE_DIM + 1) // LANES) * LANES
    places = me_s * rows + jnp.arange(rows, dtype=jnp.int32)
    part = rows // T
    begin = me_t * part
    my_places = lax.dynamic_slice(places, (begin,), (part,))
    my_latent = norm_rows(lax.dynamic_slice(latent, (begin, 0), (part, rank)), latent_gain)
    my_rope = rotate(
        lax.dynamic_slice(key_rope, (begin, 0), (part, ROPE_DIM)).astype(f32), my_places
    ).astype(bf16)
    packed = jnp.concatenate(
        [
            my_latent,
            my_rope,
            jnp.ones((part, 1), bf16),
            jnp.zeros((part, width - rank - ROPE_DIM - 1), bf16),
        ],
        axis=1,
    )
    latents = lax.all_gather(packed, ("sp", "tp"), axis=0, tiled=True)

    both = []
    for d in range(T):
        other = me_t ^ d
        piece = jnp.concatenate(
            [
                lax.dynamic_slice(expert_gate[0], (other * K, 0), (K, F)),
                lax.dynamic_slice(expert_up[0], (other * K, 0), (K, F)),
            ],
            axis=1,
        )
        if d > 0:
            piece = lax.ppermute(piece, "tp", [(i, i ^ d) for i in range(T)])
        both.append(piece)

    rot_query = rotate(
        query_rope.astype(f32).reshape(rows, heads, ROPE_DIM), places
    ).astype(bf16)
    query = jnp.concatenate(
        [
            query_nope.reshape(rows, heads, NOPE_DIM),
            rot_query,
            jnp.zeros((rows, heads, LANES - NOPE_DIM - ROPE_DIM), bf16),
        ],
        axis=2,
    ).reshape(rows, heads * LANES)
    rope_in = jnp.zeros((width - rank, LANES), bf16)
    rope_in = rope_in + jnp.asarray(
        jnp.arange(width - rank)[:, None] + NOPE_DIM == jnp.arange(LANES)[None, :]
    ).astype(bf16) * (jnp.arange(width - rank)[:, None] < ROPE_DIM).astype(bf16)
    one_in = (
        (jnp.arange(width - rank)[:, None] == ROPE_DIM)
        & (jnp.arange(LANES)[None, :] == VALUE_DIM)
    ).astype(bf16)

    def widen(weight, size, tail):
        weight = weight.reshape(rank, heads, size)
        weight = jnp.pad(weight, ((0, 0), (0, 0), (0, LANES - size))).reshape(rank, heads * LANES)
        return jnp.concatenate([weight, jnp.tile(tail, (1, heads))], axis=0)

    wk = widen(key_up, NOPE_DIM, rope_in)
    wv = widen(value_up, VALUE_DIM, one_in)
    vmem = pl.BlockSpec(memory_space=pltpu.VMEM)
    seq = S * rows
    attended = pl.pallas_call(
        functools.partial(attend_kernel, heads),
        name="attend",
        out_shape=jax.ShapeDtypeStruct((rows, heads * VALUE_DIM), bf16),
        in_specs=[vmem] * 4,
        out_specs=vmem,
        scratch_shapes=[
            pltpu.VMEM((heads, rows, LANES), f32),
            pltpu.VMEM((heads, rows, LANES), f32),
        ],
        compiler_params=pltpu.CompilerParams(vmem_limit_bytes=48 * 2**20),
        cost_estimate=pl.CostEstimate(
            flops=4 * heads * rows * seq * LANES + 4 * seq * width * heads * LANES,
            bytes_accessed=seq * width * 2,
            transcendentals=heads * rows * seq,
        ),
    )(query, latents, wk, wv)

    experts = S * expert_gate.shape[0]
    capacity = 5 * rows * TOP_K // (4 * experts)
    C = -(-capacity // 8) * 8
    M = min(S, 8 if T <= 4 else 4)
    chosen = routes[:, :, None] == jnp.arange(experts, dtype=jnp.int32)[None, None, :]
    named = jnp.sum(chosen.astype(f32), axis=1).astype(bf16)
    earlier = (jnp.arange(rows)[:, None] > jnp.arange(rows)[None, :]).astype(bf16)
    before = jnp.dot(earlier, named, preferred_element_type=f32)
    number = jnp.sum(jnp.where(chosen, before[:, None, :], 0.0), axis=2)
    slots = routes.astype(f32) * C + number
    slot_rows = jnp.transpose(slots)
    slot_cols = jnp.concatenate([slots, route_weight], axis=1)

    anywhere = pl.BlockSpec(memory_space=pl.ANY)
    dma = pltpu.SemaphoreType.DMA
    return pl.pallas_call(
        functools.partial(expert_kernel, S, T, C, M),
        name="experts",
        out_shape=jax.ShapeDtypeStruct((rows, K), bf16),
        in_specs=[vmem] * 6 + [anywhere] * (T + 1),
        out_specs=vmem,
        scratch_shapes=[
            pltpu.VMEM((T - 1, rows, heads * VALUE_DIM), bf16),
            pltpu.VMEM((8, rows), f32),
            pltpu.VMEM((T - 1, 8, rows), f32),
            pltpu.VMEM((rows, K), bf16),
            pltpu.VMEM((rows, K), f32),
            pltpu.VMEM((rows, K), bf16),
            pltpu.VMEM((S, C, K), bf16),
            pltpu.VMEM((S, C, K), bf16),
            pltpu.VMEM((S, T - 1, C, 2 * F), bf16),
            pltpu.VMEM((S, T - 1, C, 2 * F), bf16),
            pltpu.VMEM((2, C, 2 * F), f32),
            pltpu.VMEM((S, T, C, F), bf16),
            pltpu.VMEM((S, C, K), bf16),
            pltpu.VMEM((S, C, K), bf16),
            pltpu.VMEM((T, K, 2 * F), bf16),
            pltpu.VMEM(expert_down.shape[1:], bf16),
            dma((T + 1,)),
            dma((T - 1,)), dma((T - 1,)), dma((T - 1,)), dma((T - 1,)),
            dma((S,)), dma((S,)),
            dma((M, T - 1)), dma((M, T - 1)), dma((M, T - 1)), dma((M, T - 1)),
            dma((S,)), dma((S,)),
        ],
        compiler_params=pltpu.CompilerParams(
            collective_id=0, has_side_effects=True, vmem_limit_bytes=56 * 2**20
        ),
        cost_estimate=pl.CostEstimate(
            flops=6 * S * C * K * F * T, bytes_accessed=8 * K * K * 2, transcendentals=S * C * F
        ),
    )(attended, residual, out_proj, norm_gain[None, :], slot_rows, slot_cols, *both, expert_down[0])


def solution(mesh):
    in_specs = (
        P("sp", "tp"),
        P("sp", "tp"),
        P("sp", "tp"),
        P("sp", None),
        P("sp", None),
        P(),
        P(None, "tp"),
        P(None, "tp"),
        P(None, "tp"),
        P("tp"),
        P("sp", None),
        P("sp", None),
        P("sp", None, "tp"),
        P("sp", None, "tp"),
        P("sp", None, "tp"),
    )
    out_specs = P("sp", "tp")
    return jax.shard_map(
        per_device, mesh=mesh, in_specs=in_specs, out_specs=out_specs, check_vma=False
    )
```

```python
import functools

import jax
import jax.numpy as jnp
from jax import lax
from jax.experimental import pallas as pl
from jax.experimental.pallas import tpu as pltpu
from jax.sharding import PartitionSpec as P

NOPE_DIM = 64
ROPE_DIM = 32
VALUE_DIM = 64
TOP_K = 2
LANES = 128

epsilon = 1e-06
rope_base = 10000.0
negative = -1e30
MESH = pl.DeviceIdType.MESH
bf16 = jnp.bfloat16
f32 = jnp.float32


def rotate(values_in, places):
    half_dim = values_in.shape[-1] // 2
    inverse = rope_base ** (-jnp.arange(half_dim, dtype=jnp.float32) / half_dim)
    angles = places.astype(jnp.float32)[:, None] * inverse[None, :]
    angles = angles.reshape((angles.shape[0],) + (1,) * (values_in.ndim - 2) + (half_dim,))
    cosine = jnp.cos(angles)
    sine_wave = jnp.sin(angles)
    first_half = values_in[..., :half_dim]
    second_half = values_in[..., half_dim:]
    return jnp.concatenate(
        [
            first_half * cosine - second_half * sine_wave,
            first_half * sine_wave + second_half * cosine,
        ],
        axis=-1,
    )


def norm_rows(values_in, gain_vec):
    wide = values_in.astype(jnp.float32)
    mean_square = jnp.mean(wide * wide, axis=-1, keepdims=True)
    return (wide * lax.rsqrt(mean_square + epsilon) * gain_vec[None, :]).astype(jnp.bfloat16)


def flip(a, b, n):
    total = 0
    bit = 1
    while bit < n:
        total = total + ((a // bit) % 2 + (b // bit) % 2) % 2 * bit
        bit *= 2
    return total


def layer_kernel(
    S, T, C, M, heads,
    q_ref, lat_ref, wk_ref, wv_ref, spread_ref, res_ref, gain_ref, slot_ref, cols_ref,
    wo_hbm, gate_hbm, up_hbm, down_hbm,
    out_ref,
    lat_all, top_ref, sum_ref, nume_ref, att_ref,
    att_all, sq_own, sq_all, mid_ref, acc_ref, norm_ref, send, recv, psend, precv, own, hid, res, ret,
    wo_ref, gate_ref, up_ref, down_ref,
    load_sem, z_s, c_s, l_r, w_s, w_r,
    att_s, att_r, sq_s, sq_r, d_s, d_r, p_s, p_r, h_s, h_r, r_s, r_r,
):
    me_s = lax.axis_index("sp")
    me_t = lax.axis_index("tp")
    rows, K = res_ref.shape
    heads_w = att_ref.shape[1]
    F = gate_ref.shape[2]
    CORES = 2
    me_core = me_s % CORES
    me_z = me_s // CORES
    last_z = S // CORES - 1

    def weight_rows(d):
        return pl.ds(pl.multiple_of(flip(me_t, d, T) * K, K), K)

    loads = [
        pltpu.make_async_copy(wo_hbm, wo_ref, load_sem.at[0]),
        pltpu.make_async_copy(down_hbm, down_ref, load_sem.at[1]),
        pltpu.make_async_copy(gate_hbm.at[weight_rows(0), :], gate_ref.at[0], load_sem.at[2]),
        pltpu.make_async_copy(up_hbm.at[weight_rows(0), :], up_ref.at[0], load_sem.at[3]),
    ]
    for load in loads:
        load.start()

    barrier = pltpu.get_barrier_semaphore()
    for d in range(1, T):
        pl.semaphore_signal(barrier, inc=1, device_id=(me_s, flip(me_t, d, T)), device_id_type=MESH)
    for j in range(1, S):
        pl.semaphore_signal(barrier, inc=1, device_id=(flip(me_s, j, S), me_t), device_id_type=MESH)
    pl.semaphore_wait(barrier, S + T - 2)

    def remote(src, dst, ss, rs, s, t):
        return pltpu.make_async_remote_copy(
            src_ref=src, dst_ref=dst, send_sem=ss, recv_sem=rs, device_id=(s, t), device_id_type=MESH
        )

    def att_copy(d):
        return remote(att_ref, att_all.at[d - 1], att_s.at[d - 1], att_r.at[d - 1], me_s, flip(me_t, d, T))

    def sq_copy(d):
        return remote(sq_own, sq_all.at[d - 1], sq_s.at[d - 1], sq_r.at[d - 1], me_s, flip(me_t, d, T))

    def d_copy(j):
        return remote(send.at[j], recv.at[j], d_s.at[j], d_r.at[j], flip(me_s, j, S), me_t)

    def p_copy(j, d):
        return remote(
            psend.at[j, d - 1], precv.at[j, d - 1], p_s.at[j % M, d - 1], p_r.at[j % M, d - 1],
            me_s, flip(me_t, d, T),
        )

    def h_copy(j, d):
        return remote(
            hid.at[j, 0], hid.at[j, d], h_s.at[j % M, d - 1], h_r.at[j % M, d - 1], me_s, flip(me_t, d, T)
        )

    def r_copy(j):
        return remote(res.at[j], ret.at[j], r_s.at[j], r_r.at[j], flip(me_s, j, S), me_t)

    def gate_copy(d):
        return remote(
            gate_hbm.at[weight_rows(d), :], gate_ref.at[d], w_s.at[0, d - 1], w_r.at[0, d - 1],
            me_s, flip(me_t, d, T),
        )

    def up_copy(d):
        return remote(
            up_hbm.at[weight_rows(d), :], up_ref.at[d], w_s.at[1, d - 1], w_r.at[1, d - 1],
            me_s, flip(me_t, d, T),
        )

    def own_up():
        return remote(lat_ref, lat_all.at[me_s], z_s.at[me_s], l_r.at[me_s], me_s + CORES, me_t)

    def own_across():
        return remote(lat_ref, lat_all.at[me_s], c_s.at[me_s], l_r.at[me_s], me_s + 1, me_t)

    def pass_up(b):
        return remote(lat_all.at[b], lat_all.at[b], z_s.at[b], l_r.at[b], me_s + CORES, me_t)

    def pass_across(b):
        return remote(
            lat_all.at[b], lat_all.at[b], c_s.at[b], l_r.at[b], me_s + 1 - 2 * me_core, me_t
        )

    @pl.when(me_z < last_z)
    def _():
        own_up().start()

    @pl.when(me_core == 0)
    def _():
        own_across().start()

    for d in range(1, T):
        gate_copy(d).start()
        up_copy(d).start()

    scale = (NOPE_DIM + ROPE_DIM) ** (-0.5) * 1.4426950408889634
    top_ref[...] = jnp.full(top_ref.shape, negative, f32)
    nume_ref[...] = jnp.zeros(nume_ref.shape, f32)
    sum_ref[...] = jnp.zeros(sum_ref.shape, f32)
    rank = lat_ref.shape[1]
    folds = rank // ROPE_DIM

    def attend(block, masked):
        lat = block[:rows, :]
        packed = block[rows:, :].astype(f32)
        rope = jnp.concatenate(
            [packed[:, q * ROPE_DIM : (q + 1) * ROPE_DIM] for q in range(folds)], axis=0
        ).astype(bf16)
        keys = (
            jnp.dot(lat, wk_ref[...], preferred_element_type=f32)
            + jnp.dot(rope, spread_ref[...], preferred_element_type=f32)
        ).astype(bf16)
        values = jnp.dot(lat, wv_ref[...], preferred_element_type=f32).astype(bf16)
        for h in range(heads):
            cols = slice(h * LANES, (h + 1) * LANES)
            scores = lax.dot_general(
                q_ref[:, cols], keys[:, cols], (((1,), (1,)), ((), ())), preferred_element_type=f32
            )
            if masked:
                allowed = lax.broadcasted_iota(jnp.int32, scores.shape, 1) <= (
                    lax.broadcasted_iota(jnp.int32, scores.shape, 0)
                )
                scores = jnp.where(allowed, scores, negative)
            old = top_ref[h]
            new = jnp.maximum(old, jnp.max(scores, axis=1, keepdims=True))
            weights = jnp.exp2((scores - new[:, :1]) * scale)
            fading = jnp.exp2((old - new) * scale)
            top_ref[h] = new
            sum_ref[h] = sum_ref[h] * fading + jnp.sum(weights, axis=1, keepdims=True)
            nume_ref[h] = nume_ref[h] * fading + jnp.dot(
                weights.astype(bf16), values[:, cols], preferred_element_type=f32
            )

    attend(lat_ref[...], True)

    @pl.when(me_core == 1)
    def _():
        pass_across(me_s - 1).wait_recv()
        attend(lat_all[me_s - 1], False)

    @pl.loop(1, me_z + 1)
    def _(k):
        b = me_s - CORES * k
        pass_across(b).wait_recv()

        @pl.when(me_z < last_z)
        def _():
            pass_up(b).start()

        pass_across(b).start()
        attend(lat_all[b], False)
        other = b + 1 - 2 * me_core
        pass_across(other).wait_recv()
        attend(lat_all[other], False)

    outs = []
    for h in range(heads):
        outs.append(nume_ref[h][:, :VALUE_DIM] / sum_ref[h][:, :1])
    att_ref[...] = jnp.concatenate(outs, axis=1).astype(bf16)
    for d in range(1, T):
        att_copy(d).start()
    loads[0].wait()

    def project(att, d):
        begin = pl.multiple_of(flip(me_t, d, T) * heads_w, heads_w)
        return jnp.dot(att, wo_ref[pl.ds(begin, heads_w), :], preferred_element_type=f32)

    acc_ref[...] = res_ref[...].astype(f32) + project(att_ref[...], 0)
    for d in range(1, T):
        att_copy(d).wait_recv()
        acc_ref[...] += project(att_all[d - 1], d)
    mid_ref[...] = acc_ref[...].astype(bf16)
    wide = mid_ref[...].astype(f32)
    square = jnp.sum(wide * wide, axis=1, keepdims=True)
    sq_own[...] = jnp.transpose(jnp.broadcast_to(square, (rows, LANES)))[:8]
    for d in range(1, T):
        sq_copy(d).start()
    total = sq_own[...]
    for d in range(1, T):
        sq_copy(d).wait_recv()
        total = total + sq_all[d - 1]
    row_scale = lax.rsqrt(total / (K * T) + epsilon)
    row_scale = jnp.transpose(jnp.broadcast_to(row_scale[:1], (LANES, rows)))[:, :1]
    wide = mid_ref[...].astype(f32)
    norm_ref[...] = (wide * row_scale * gain_ref[...]).astype(bf16)
    acc_ref[...] = wide

    def rows_for(j):
        base = (flip(me_s, j, S) * C).astype(f32)
        places = lax.broadcasted_iota(jnp.int32, (C, rows), 0).astype(f32) + base
        hit = (places == slot_ref[0:1, :]) | (places == slot_ref[1:2, :])
        picks = jnp.where(hit, 1.0, 0.0).astype(bf16)
        return jnp.dot(picks, norm_ref[...], preferred_element_type=f32).astype(bf16)

    @pl.loop(1, S)
    def _(j):
        send[j] = rows_for(j)
        d_copy(j).start()

    recv[0] = rows_for(0)
    for load in loads[1:]:
        load.wait()
    for d in range(1, T):
        gate_copy(d).wait_recv()
        up_copy(d).wait_recv()

    def add_result(j):
        base = (flip(me_s, j, S) * C).astype(f32)
        places = lax.broadcasted_iota(jnp.int32, (rows, C), 1).astype(f32) + base
        hit0 = places == cols_ref[:, 0:1]
        hit1 = places == cols_ref[:, 1:2]
        picks = jnp.where(hit0 | hit1, 1.0, 0.0).astype(bf16)
        inside0 = (cols_ref[:, 0:1] >= base) & (cols_ref[:, 0:1] < base + C)
        inside1 = (cols_ref[:, 1:2] >= base) & (cols_ref[:, 1:2] < base + C)
        share = jnp.where(inside0, cols_ref[:, 2:3], jnp.where(inside1, cols_ref[:, 3:4], 0.0))
        acc_ref[...] += share * jnp.dot(picks, ret[j], preferred_element_type=f32)

    @pl.loop(0, S + 2)
    def _(i):
        @pl.when(i < S)
        def _():
            j = i

            @pl.when(j > 0)
            def _():
                d_copy(j).wait_recv()

            block = recv[j]
            for d in range(1, T):
                if S > M:

                    @pl.when(j >= M)
                    def _():
                        p_copy(j - M, d).wait_send()

                psend[j, d - 1, :, :F] = jnp.dot(
                    block, gate_ref[d], preferred_element_type=f32
                ).astype(bf16)
                psend[j, d - 1, :, F:] = jnp.dot(
                    block, up_ref[d], preferred_element_type=f32
                ).astype(bf16)
                p_copy(j, d).start()
            own[j % 2, :, :F] = jnp.dot(block, gate_ref[0], preferred_element_type=f32)
            own[j % 2, :, F:] = jnp.dot(block, up_ref[0], preferred_element_type=f32)

        @pl.when((i >= 1) & (i < S + 1))
        def _():
            j = i - 1
            total = own[j % 2]
            for d in range(1, T):
                p_copy(j, d).wait_recv()
                total = total + precv[j, d - 1].astype(f32)
            gate = total[:, :F]
            hid[j, 0] = (gate / (1.0 + jnp.exp(-gate)) * total[:, F:]).astype(bf16)
            for d in range(1, T):
                if S > M:

                    @pl.when(j >= M)
                    def _():
                        h_copy(j - M, d).wait_send()

                h_copy(j, d).start()

        @pl.when(i >= 2)
        def _():
            j = i - 2
            total = jnp.zeros((C, K), f32)
            for d in range(T):
                if d > 0:
                    h_copy(j, d).wait_recv()
                begin = pl.multiple_of(flip(me_t, d, T) * F, F)
                total += jnp.dot(hid[j, d], down_ref[pl.ds(begin, F), :], preferred_element_type=f32)

            @pl.when(j > 0)
            def _():
                res[j] = total.astype(bf16)
                r_copy(j).start()

            @pl.when(j == 0)
            def _():
                ret[j] = total.astype(bf16)

    add_result(0)

    @pl.loop(1, S)
    def _(j):
        r_copy(j).wait_recv()
        add_result(j)

    out_ref[...] = acc_ref[...].astype(bf16)

    @pl.when(me_z < last_z)
    def _():
        own_up().wait_send()

    @pl.when(me_core == 0)
    def _():
        own_across().wait_send()

    @pl.loop(1, me_z + 1)
    def _(k):
        b = me_s - CORES * k

        @pl.when(me_z < last_z)
        def _():
            pass_up(b).wait_send()

        pass_across(b).wait_send()

    for d in range(1, T):
        gate_copy(d).wait_send()
        up_copy(d).wait_send()
        att_copy(d).wait_send()
        sq_copy(d).wait_send()

    @pl.loop(S - M, S)
    def _(j):
        for d in range(1, T):
            p_copy(j, d).wait_send()
            h_copy(j, d).wait_send()

    @pl.loop(1, S)
    def _(j):
        d_copy(j).wait_send()
        r_copy(j).wait_send()


def per_device(
    residual, query_nope, query_rope, latent, key_rope, latent_gain, key_up, value_up, out_proj,
    norm_gain, routes, route_weight, expert_gate, expert_up, expert_down,
):
    rows, K = residual.shape
    S = lax.axis_size("sp")
    T = lax.axis_size("tp")
    me_s = lax.axis_index("sp")
    me_t = lax.axis_index("tp")
    heads = query_nope.shape[1] // NOPE_DIM
    rank = latent.shape[1]
    F = expert_gate.shape[2]

    places = me_s * rows + jnp.arange(rows, dtype=jnp.int32)
    folds = rank // ROPE_DIM
    rot_key = rotate(key_rope.astype(f32), places).astype(bf16)
    folded = jnp.swapaxes(rot_key.reshape(folds, rows // folds, ROPE_DIM), 0, 1)
    packed = jnp.concatenate(
        [norm_rows(latent, latent_gain), folded.reshape(rows // folds, rank)], axis=0
    )

    rot_query = rotate(
        query_rope.astype(f32).reshape(rows, heads, ROPE_DIM), places
    ).astype(bf16)
    query = jnp.concatenate(
        [
            query_nope.reshape(rows, heads, NOPE_DIM),
            rot_query,
            jnp.zeros((rows, heads, LANES - NOPE_DIM - ROPE_DIM), bf16),
        ],
        axis=2,
    ).reshape(rows, heads * LANES)
    spread = jnp.tile(
        (jnp.arange(ROPE_DIM)[:, None] + NOPE_DIM == jnp.arange(LANES)[None, :]).astype(bf16),
        (1, heads),
    )

    def widen(weight, size):
        weight = weight.reshape(rank, heads, size)
        return jnp.pad(weight, ((0, 0), (0, 0), (0, LANES - size))).reshape(rank, heads * LANES)

    wk = widen(key_up, NOPE_DIM)
    wv = widen(value_up, VALUE_DIM)
    vmem = pl.BlockSpec(memory_space=pltpu.VMEM)

    experts = S * expert_gate.shape[0]
    capacity = 5 * rows * TOP_K // (4 * experts)
    C = -(-capacity // 8) * 8
    M = min(S, 8 if T <= 4 else 4)
    chosen = routes[:, :, None] == jnp.arange(experts, dtype=jnp.int32)[None, None, :]
    named = jnp.sum(chosen.astype(f32), axis=1).astype(bf16)
    earlier = (jnp.arange(rows)[:, None] > jnp.arange(rows)[None, :]).astype(bf16)
    before = jnp.dot(earlier, named, preferred_element_type=f32)
    number = jnp.sum(jnp.where(chosen, before[:, None, :], 0.0), axis=2)
    slots = routes.astype(f32) * C + number
    slot_rows = jnp.transpose(slots)
    slot_cols = jnp.concatenate([slots, route_weight], axis=1)

    anywhere = pl.BlockSpec(memory_space=pl.ANY)
    dma = pltpu.SemaphoreType.DMA
    return pl.pallas_call(
        functools.partial(layer_kernel, S, T, C, M, heads),
        name="layer",
        out_shape=jax.ShapeDtypeStruct((rows, K), bf16),
        in_specs=[vmem] * 9 + [anywhere] * 4,
        out_specs=vmem,
        scratch_shapes=[
            pltpu.VMEM((S,) + packed.shape, bf16),
            pltpu.VMEM((heads, rows, LANES), f32),
            pltpu.VMEM((heads, rows, LANES), f32),
            pltpu.VMEM((heads, rows, LANES), f32),
            pltpu.VMEM((rows, heads * VALUE_DIM), bf16),
            pltpu.VMEM((T - 1, rows, heads * VALUE_DIM), bf16),
            pltpu.VMEM((8, rows), f32),
            pltpu.VMEM((T - 1, 8, rows), f32),
            pltpu.VMEM((rows, K), bf16),
            pltpu.VMEM((rows, K), f32),
            pltpu.VMEM((rows, K), bf16),
            pltpu.VMEM((S, C, K), bf16),
            pltpu.VMEM((S, C, K), bf16),
            pltpu.VMEM((S, T - 1, C, 2 * F), bf16),
            pltpu.VMEM((S, T - 1, C, 2 * F), bf16),
            pltpu.VMEM((2, C, 2 * F), f32),
            pltpu.VMEM((S, T, C, F), bf16),
            pltpu.VMEM((S, C, K), bf16),
            pltpu.VMEM((S, C, K), bf16),
            pltpu.VMEM(out_proj.shape, bf16),
            pltpu.VMEM((T, K, F), bf16),
            pltpu.VMEM((T, K, F), bf16),
            pltpu.VMEM(expert_down.shape[1:], bf16),
            dma((4,)),
            dma((S,)), dma((S,)), dma((S,)), dma((2, T - 1)), dma((2, T - 1)),
            dma((T - 1,)), dma((T - 1,)), dma((T - 1,)), dma((T - 1,)),
            dma((S,)), dma((S,)),
            dma((M, T - 1)), dma((M, T - 1)), dma((M, T - 1)), dma((M, T - 1)),
            dma((S,)), dma((S,)),
        ],
        compiler_params=pltpu.CompilerParams(
            collective_id=0, has_side_effects=True, vmem_limit_bytes=56 * 2**20
        ),
        cost_estimate=pl.CostEstimate(
            flops=6 * S * C * K * F * T, bytes_accessed=8 * K * K * 2, transcendentals=S * C * F
        ),
    )(
        query, packed, wk, wv, spread, residual, norm_gain[None, :], slot_rows, slot_cols,
        out_proj, expert_gate[0], expert_up[0], expert_down[0],
    )


def solution(mesh):
    in_specs = (
        P("sp", "tp"),
        P("sp", "tp"),
        P("sp", "tp"),
        P("sp", None),
        P("sp", None),
        P(),
        P(None, "tp"),
        P(None, "tp"),
        P(None, "tp"),
        P("tp"),
        P("sp", None),
        P("sp", None),
        P("sp", None, "tp"),
        P("sp", None, "tp"),
        P("sp", None, "tp"),
    )
    out_specs = P("sp", "tp")
    return jax.shard_map(
        per_device, mesh=mesh, in_specs=in_specs, out_specs=out_specs, check_vma=False
    )
```

```python
import functools

import jax
import jax.numpy as jnp
from jax import lax
from jax.experimental import pallas as pl
from jax.experimental.pallas import tpu as pltpu
from jax.sharding import PartitionSpec as P

NOPE_DIM = 64
ROPE_DIM = 32
VALUE_DIM = 64
TOP_K = 2
LANES = 128

epsilon = 1e-06
rope_base = 10000.0
negative = -1e30
MESH = pl.DeviceIdType.MESH
bf16 = jnp.bfloat16
f32 = jnp.float32


def flip(a, b, n):
    total = 0
    bit = 1
    while bit < n:
        total = total + ((a // bit) % 2 + (b // bit) % 2) % 2 * bit
        bit *= 2
    return total


def layer_kernel(
    S, T, C, M, heads,
    nope_ref, turn_ref, cos_ref, sin_ref, latent_ref, lat_gain_ref, ku_ref, vu_ref, res_ref, gain_ref, slot_ref, cols_ref,
    wo_hbm, gate_hbm, up_hbm, down_hbm,
    out_ref,
    q_ref, lat_ref, wk_ref, wv_ref, lat_all, top_ref, sum_ref, nume_ref, att_ref,
    att_all, sq_own, sq_all, mid_ref, acc_ref, norm_ref, send, recv, psend, precv, own, hid, res, ret,
    wo_ref, gate_ref, up_ref, down_ref,
    load_sem, z_s, c_s, l_r, w_s, w_r,
    att_s, att_r, sq_s, sq_r, d_s, d_r, p_s, p_r, h_s, h_r, r_s, r_r,
):
    me_s = lax.axis_index("sp")
    me_t = lax.axis_index("tp")
    rows, K = res_ref.shape
    heads_w = att_ref.shape[1]
    F = gate_ref.shape[2]
    CORES = 2
    me_core = me_s % CORES
    me_z = me_s // CORES
    last_z = S // CORES - 1

    def weight_rows(d):
        return pl.ds(pl.multiple_of(flip(me_t, d, T) * K, K), K)

    loads = [
        pltpu.make_async_copy(wo_hbm, wo_ref, load_sem.at[0]),
        pltpu.make_async_copy(down_hbm, down_ref, load_sem.at[1]),
        pltpu.make_async_copy(gate_hbm.at[weight_rows(0), :], gate_ref.at[0], load_sem.at[2]),
        pltpu.make_async_copy(up_hbm.at[weight_rows(0), :], up_ref.at[0], load_sem.at[3]),
    ]
    for load in loads:
        load.start()

    wide = latent_ref[...].astype(f32)
    mean_square = jnp.mean(wide * wide, axis=1, keepdims=True)
    lat_ref[:rows, :] = (wide * lax.rsqrt(mean_square + epsilon) * lat_gain_ref[...]).astype(bf16)
    rank = latent_ref.shape[1]
    folds = rank // ROPE_DIM
    fold_rows = rows // folds
    width = turn_ref.shape[1]
    swap = lax.broadcasted_iota(jnp.int32, (width, width), 0) == (
        lax.broadcasted_iota(jnp.int32, (width, width), 1) ^ (ROPE_DIM // 2)
    )
    partner = jnp.dot(
        turn_ref[...], jnp.where(swap, 1.0, 0.0).astype(bf16), preferred_element_type=f32
    )
    turned = turn_ref[...].astype(f32) * cos_ref[...] + partner * sin_ref[...]
    key_turned = turned[:, heads * ROPE_DIM : (heads + 1) * ROPE_DIM]
    lat_ref[rows:, :] = jnp.concatenate(
        [key_turned[q * fold_rows : (q + 1) * fold_rows, :] for q in range(folds)], axis=1
    ).astype(bf16)

    barrier = pltpu.get_barrier_semaphore()
    for d in range(1, T):
        pl.semaphore_signal(barrier, inc=1, device_id=(me_s, flip(me_t, d, T)), device_id_type=MESH)
    for j in range(1, S):
        pl.semaphore_signal(barrier, inc=1, device_id=(flip(me_s, j, S), me_t), device_id_type=MESH)
    pl.semaphore_wait(barrier, S + T - 2)

    def remote(src, dst, ss, rs, s, t):
        return pltpu.make_async_remote_copy(
            src_ref=src, dst_ref=dst, send_sem=ss, recv_sem=rs, device_id=(s, t), device_id_type=MESH
        )

    def att_copy(d):
        return remote(att_ref, att_all.at[d - 1], att_s.at[d - 1], att_r.at[d - 1], me_s, flip(me_t, d, T))

    def sq_copy(d):
        return remote(sq_own, sq_all.at[d - 1], sq_s.at[d - 1], sq_r.at[d - 1], me_s, flip(me_t, d, T))

    def d_copy(j):
        return remote(send.at[j], recv.at[j], d_s.at[j], d_r.at[j], flip(me_s, j, S), me_t)

    def p_copy(j, d):
        return remote(
            psend.at[j, d - 1], precv.at[j, d - 1], p_s.at[j % M, d - 1], p_r.at[j % M, d - 1],
            me_s, flip(me_t, d, T),
        )

    def h_copy(j, d):
        return remote(
            hid.at[j, 0], hid.at[j, d], h_s.at[j % M, d - 1], h_r.at[j % M, d - 1], me_s, flip(me_t, d, T)
        )

    def r_copy(j):
        return remote(res.at[j], ret.at[j], r_s.at[j], r_r.at[j], flip(me_s, j, S), me_t)

    def gate_copy(d):
        return remote(
            gate_hbm.at[weight_rows(d), :], gate_ref.at[d], w_s.at[0, d - 1], w_r.at[0, d - 1],
            me_s, flip(me_t, d, T),
        )

    def up_copy(d):
        return remote(
            up_hbm.at[weight_rows(d), :], up_ref.at[d], w_s.at[1, d - 1], w_r.at[1, d - 1],
            me_s, flip(me_t, d, T),
        )

    def own_up():
        return remote(lat_ref, lat_all.at[me_s], z_s.at[me_s], l_r.at[me_s], me_s + CORES, me_t)

    def own_across():
        return remote(lat_ref, lat_all.at[me_s], c_s.at[me_s], l_r.at[me_s], me_s + 1, me_t)

    def pass_up(b):
        return remote(lat_all.at[b], lat_all.at[b], z_s.at[b], l_r.at[b], me_s + CORES, me_t)

    def pass_across(b):
        return remote(
            lat_all.at[b], lat_all.at[b], c_s.at[b], l_r.at[b], me_s + 1 - 2 * me_core, me_t
        )

    @pl.when(me_z < last_z)
    def _():
        own_up().start()

    @pl.when(me_core == 0)
    def _():
        own_across().start()

    for d in range(1, T):
        gate_copy(d).start()

    def spaced(parts):
        return jnp.concatenate(parts, axis=1).astype(bf16)

    for h in range(heads):
        cols = slice(h * LANES, (h + 1) * LANES)
        q_ref[:, cols] = spaced(
            [
                nope_ref[:, h * NOPE_DIM : (h + 1) * NOPE_DIM].astype(f32),
                turned[:, h * ROPE_DIM : (h + 1) * ROPE_DIM],
                jnp.zeros((rows, LANES - NOPE_DIM - ROPE_DIM), f32),
            ]
        )
        wk_ref[:, cols] = spaced(
            [
                ku_ref[:, h * NOPE_DIM : (h + 1) * NOPE_DIM].astype(f32),
                jnp.zeros((rank, LANES - NOPE_DIM), f32),
            ]
        )
        wv_ref[:, cols] = spaced(
            [
                vu_ref[:, h * VALUE_DIM : (h + 1) * VALUE_DIM].astype(f32),
                jnp.zeros((rank, LANES - VALUE_DIM), f32),
            ]
        )
    spread = jnp.where(
        lax.broadcasted_iota(jnp.int32, (ROPE_DIM, heads * LANES), 0) + NOPE_DIM
        == lax.broadcasted_iota(jnp.int32, (ROPE_DIM, heads * LANES), 1) % LANES,
        1.0,
        0.0,
    ).astype(bf16)

    scale = (NOPE_DIM + ROPE_DIM) ** (-0.5) * 1.4426950408889634
    top_ref[...] = jnp.full(top_ref.shape, negative, f32)
    nume_ref[...] = jnp.zeros(nume_ref.shape, f32)
    sum_ref[...] = jnp.zeros(sum_ref.shape, f32)

    def attend(block, masked):
        lat = block[:rows, :]
        packed = block[rows:, :].astype(f32)
        rope = jnp.concatenate(
            [packed[:, q * ROPE_DIM : (q + 1) * ROPE_DIM] for q in range(folds)], axis=0
        ).astype(bf16)
        keys = (
            jnp.dot(lat, wk_ref[...], preferred_element_type=f32)
            + jnp.dot(rope, spread, preferred_element_type=f32)
        ).astype(bf16)
        values = jnp.dot(lat, wv_ref[...], preferred_element_type=f32).astype(bf16)
        for h in range(heads):
            cols = slice(h * LANES, (h + 1) * LANES)
            scores = lax.dot_general(
                q_ref[:, cols], keys[:, cols], (((1,), (1,)), ((), ())), preferred_element_type=f32
            )
            if masked:
                allowed = lax.broadcasted_iota(jnp.int32, scores.shape, 1) <= (
                    lax.broadcasted_iota(jnp.int32, scores.shape, 0)
                )
                scores = jnp.where(allowed, scores, negative)
            old = top_ref[h]
            new = jnp.maximum(old, jnp.max(scores, axis=1, keepdims=True))
            weights = jnp.exp2((scores - new[:, :1]) * scale)
            fading = jnp.exp2((old - new) * scale)
            top_ref[h] = new
            sum_ref[h] = sum_ref[h] * fading + jnp.sum(weights, axis=1, keepdims=True)
            nume_ref[h] = nume_ref[h] * fading + jnp.dot(
                weights.astype(bf16), values[:, cols], preferred_element_type=f32
            )

    attend(lat_ref[...], True)

    @pl.when(me_core == 1)
    def _():
        pass_across(me_s - 1).wait_recv()
        attend(lat_all[me_s - 1], False)

    @pl.loop(1, me_z + 1)
    def _(k):
        b = me_s - CORES * k
        pass_across(b).wait_recv()

        @pl.when(me_z < last_z)
        def _():
            pass_up(b).start()

        pass_across(b).start()
        attend(lat_all[b], False)
        other = b + 1 - 2 * me_core
        pass_across(other).wait_recv()
        attend(lat_all[other], False)

    outs = []
    for h in range(heads):
        outs.append(nume_ref[h][:, :VALUE_DIM] / sum_ref[h][:, :1])
    att_ref[...] = jnp.concatenate(outs, axis=1).astype(bf16)
    for d in range(1, T):
        att_copy(d).start()
    for d in range(1, T):
        up_copy(d).start()
    loads[0].wait()

    def project(att, d):
        begin = pl.multiple_of(flip(me_t, d, T) * heads_w, heads_w)
        return jnp.dot(att, wo_ref[pl.ds(begin, heads_w), :], preferred_element_type=f32)

    acc_ref[...] = res_ref[...].astype(f32) + project(att_ref[...], 0)
    for d in range(1, T):
        att_copy(d).wait_recv()
        acc_ref[...] += project(att_all[d - 1], d)
    mid_ref[...] = acc_ref[...].astype(bf16)
    wide = mid_ref[...].astype(f32)
    square = jnp.sum(wide * wide, axis=1, keepdims=True)
    sq_own[...] = jnp.transpose(jnp.broadcast_to(square, (rows, LANES)))[:8]
    for d in range(1, T):
        sq_copy(d).start()
    total = sq_own[...]
    for d in range(1, T):
        sq_copy(d).wait_recv()
        total = total + sq_all[d - 1]
    row_scale = lax.rsqrt(total / (K * T) + epsilon)
    row_scale = jnp.transpose(jnp.broadcast_to(row_scale[:1], (LANES, rows)))[:, :1]
    wide = mid_ref[...].astype(f32)
    norm_ref[...] = (wide * row_scale * gain_ref[...]).astype(bf16)
    acc_ref[...] = wide

    def rows_for(j):
        base = (flip(me_s, j, S) * C).astype(f32)
        places = lax.broadcasted_iota(jnp.int32, (C, rows), 0).astype(f32) + base
        hit = (places == slot_ref[0:1, :]) | (places == slot_ref[1:2, :])
        picks = jnp.where(hit, 1.0, 0.0).astype(bf16)
        return jnp.dot(picks, norm_ref[...], preferred_element_type=f32).astype(bf16)

    @pl.loop(1, S)
    def _(j):
        send[j] = rows_for(j)
        d_copy(j).start()

    recv[0] = rows_for(0)
    for load in loads[1:]:
        load.wait()
    for d in range(1, T):
        gate_copy(d).wait_recv()
        up_copy(d).wait_recv()

    def add_result(j):
        base = (flip(me_s, j, S) * C).astype(f32)
        places = lax.broadcasted_iota(jnp.int32, (rows, C), 1).astype(f32) + base
        hit0 = places == cols_ref[:, 0:1]
        hit1 = places == cols_ref[:, 1:2]
        picks = jnp.where(hit0 | hit1, 1.0, 0.0).astype(bf16)
        inside0 = (cols_ref[:, 0:1] >= base) & (cols_ref[:, 0:1] < base + C)
        inside1 = (cols_ref[:, 1:2] >= base) & (cols_ref[:, 1:2] < base + C)
        share = jnp.where(inside0, cols_ref[:, 2:3], jnp.where(inside1, cols_ref[:, 3:4], 0.0))
        acc_ref[...] += share * jnp.dot(picks, ret[j], preferred_element_type=f32)

    @pl.loop(0, S + 2)
    def _(i):
        @pl.when(i < S)
        def _():
            j = i

            @pl.when(j > 0)
            def _():
                d_copy(j).wait_recv()

            block = recv[j]
            for d in range(1, T):
                if S > M:

                    @pl.when(j >= M)
                    def _():
                        p_copy(j - M, d).wait_send()

                psend[j, d - 1, :, :F] = jnp.dot(
                    block, gate_ref[d], preferred_element_type=f32
                ).astype(bf16)
                psend[j, d - 1, :, F:] = jnp.dot(
                    block, up_ref[d], preferred_element_type=f32
                ).astype(bf16)
                p_copy(j, d).start()
            own[j % 2, :, :F] = jnp.dot(block, gate_ref[0], preferred_element_type=f32)
            own[j % 2, :, F:] = jnp.dot(block, up_ref[0], preferred_element_type=f32)

        @pl.when((i >= 1) & (i < S + 1))
        def _():
            j = i - 1
            total = own[j % 2]
            for d in range(1, T):
                p_copy(j, d).wait_recv()
                total = total + precv[j, d - 1].astype(f32)
            gate = total[:, :F]
            hid[j, 0] = (gate / (1.0 + jnp.exp(-gate)) * total[:, F:]).astype(bf16)
            for d in range(1, T):
                if S > M:

                    @pl.when(j >= M)
                    def _():
                        h_copy(j - M, d).wait_send()

                h_copy(j, d).start()

        @pl.when(i >= 2)
        def _():
            j = i - 2
            total = jnp.zeros((C, K), f32)
            for d in range(T):
                if d > 0:
                    h_copy(j, d).wait_recv()
                begin = pl.multiple_of(flip(me_t, d, T) * F, F)
                total += jnp.dot(hid[j, d], down_ref[pl.ds(begin, F), :], preferred_element_type=f32)

            @pl.when(j > 0)
            def _():
                res[j] = total.astype(bf16)
                r_copy(j).start()

            @pl.when(j == 0)
            def _():
                ret[j] = total.astype(bf16)

    add_result(0)

    @pl.loop(1, S)
    def _(j):
        r_copy(j).wait_recv()
        add_result(j)

    out_ref[...] = acc_ref[...].astype(bf16)

    @pl.when(me_z < last_z)
    def _():
        own_up().wait_send()

    @pl.when(me_core == 0)
    def _():
        own_across().wait_send()

    @pl.loop(1, me_z + 1)
    def _(k):
        b = me_s - CORES * k

        @pl.when(me_z < last_z)
        def _():
            pass_up(b).wait_send()

        pass_across(b).wait_send()

    for d in range(1, T):
        gate_copy(d).wait_send()
        up_copy(d).wait_send()
        att_copy(d).wait_send()
        sq_copy(d).wait_send()

    @pl.loop(S - M, S)
    def _(j):
        for d in range(1, T):
            p_copy(j, d).wait_send()
            h_copy(j, d).wait_send()

    @pl.loop(1, S)
    def _(j):
        d_copy(j).wait_send()
        r_copy(j).wait_send()


def per_device(
    residual, query_nope, query_rope, latent, key_rope, latent_gain, key_up, value_up, out_proj,
    norm_gain, routes, route_weight, expert_gate, expert_up, expert_down,
):
    rows, K = residual.shape
    S = lax.axis_size("sp")
    T = lax.axis_size("tp")
    me_s = lax.axis_index("sp")
    me_t = lax.axis_index("tp")
    heads = query_nope.shape[1] // NOPE_DIM
    rank = latent.shape[1]
    F = expert_gate.shape[2]

    width = -(-(heads + 1) * ROPE_DIM // LANES) * LANES
    half = ROPE_DIM // 2
    places = me_s * rows + jnp.arange(rows, dtype=jnp.int32)
    lane = jnp.arange(width, dtype=jnp.int32)
    inverse = rope_base ** (-(lane % half).astype(f32) / half)
    angles = places.astype(f32)[:, None] * inverse[None, :]
    cosine = jnp.cos(angles)
    sine = jnp.where((lane % ROPE_DIM < half)[None, :], -jnp.sin(angles), jnp.sin(angles))
    turn = jnp.concatenate(
        [query_rope, key_rope, jnp.zeros((rows, width - (heads + 1) * ROPE_DIM), bf16)], axis=1
    )
    pack_shape = (rows + rows * ROPE_DIM // rank, rank)
    vmem = pl.BlockSpec(memory_space=pltpu.VMEM)

    experts = S * expert_gate.shape[0]
    capacity = 5 * rows * TOP_K // (4 * experts)
    C = -(-capacity // 8) * 8
    M = min(S, 8 if T <= 4 else 4)
    chosen = routes[:, :, None] == jnp.arange(experts, dtype=jnp.int32)[None, None, :]
    named = jnp.sum(chosen.astype(f32), axis=1).astype(bf16)
    earlier = (jnp.arange(rows)[:, None] > jnp.arange(rows)[None, :]).astype(bf16)
    before = jnp.dot(earlier, named, preferred_element_type=f32)
    number = jnp.sum(jnp.where(chosen, before[:, None, :], 0.0), axis=2)
    slots = routes.astype(f32) * C + number
    slot_rows = jnp.transpose(slots)
    slot_cols = jnp.concatenate([slots, route_weight], axis=1)

    anywhere = pl.BlockSpec(memory_space=pl.ANY)
    dma = pltpu.SemaphoreType.DMA
    return pl.pallas_call(
        functools.partial(layer_kernel, S, T, C, M, heads),
        name="layer",
        out_shape=jax.ShapeDtypeStruct((rows, K), bf16),
        in_specs=[vmem] * 12 + [anywhere] * 4,
        out_specs=vmem,
        scratch_shapes=[
            pltpu.VMEM((rows, heads * LANES), bf16),
            pltpu.VMEM(pack_shape, bf16),
            pltpu.VMEM((rank, heads * LANES), bf16),
            pltpu.VMEM((rank, heads * LANES), bf16),
            pltpu.VMEM((S,) + pack_shape, bf16),
            pltpu.VMEM((heads, rows, LANES), f32),
            pltpu.VMEM((heads, rows, LANES), f32),
            pltpu.VMEM((heads, rows, LANES), f32),
            pltpu.VMEM((rows, heads * VALUE_DIM), bf16),
            pltpu.VMEM((T - 1, rows, heads * VALUE_DIM), bf16),
            pltpu.VMEM((8, rows), f32),
            pltpu.VMEM((T - 1, 8, rows), f32),
            pltpu.VMEM((rows, K), bf16),
            pltpu.VMEM((rows, K), f32),
            pltpu.VMEM((rows, K), bf16),
            pltpu.VMEM((S, C, K), bf16),
            pltpu.VMEM((S, C, K), bf16),
            pltpu.VMEM((S, T - 1, C, 2 * F), bf16),
            pltpu.VMEM((S, T - 1, C, 2 * F), bf16),
            pltpu.VMEM((2, C, 2 * F), f32),
            pltpu.VMEM((S, T, C, F), bf16),
            pltpu.VMEM((S, C, K), bf16),
            pltpu.VMEM((S, C, K), bf16),
            pltpu.VMEM(out_proj.shape, bf16),
            pltpu.VMEM((T, K, F), bf16),
            pltpu.VMEM((T, K, F), bf16),
            pltpu.VMEM(expert_down.shape[1:], bf16),
            dma((4,)),
            dma((S,)), dma((S,)), dma((S,)), dma((2, T - 1)), dma((2, T - 1)),
            dma((T - 1,)), dma((T - 1,)), dma((T - 1,)), dma((T - 1,)),
            dma((S,)), dma((S,)),
            dma((M, T - 1)), dma((M, T - 1)), dma((M, T - 1)), dma((M, T - 1)),
            dma((S,)), dma((S,)),
        ],
        compiler_params=pltpu.CompilerParams(
            collective_id=0, has_side_effects=True, vmem_limit_bytes=56 * 2**20
        ),
        cost_estimate=pl.CostEstimate(
            flops=6 * S * C * K * F * T, bytes_accessed=8 * K * K * 2, transcendentals=S * C * F
        ),
    )(
        query_nope, turn, cosine, sine, latent, latent_gain[None, :], key_up, value_up, residual, norm_gain[None, :], slot_rows, slot_cols,
        out_proj, expert_gate[0], expert_up[0], expert_down[0],
    )


def solution(mesh):
    in_specs = (
        P("sp", "tp"),
        P("sp", "tp"),
        P("sp", "tp"),
        P("sp", None),
        P("sp", None),
        P(),
        P(None, "tp"),
        P(None, "tp"),
        P(None, "tp"),
        P("tp"),
        P("sp", None),
        P("sp", None),
        P("sp", None, "tp"),
        P("sp", None, "tp"),
        P("sp", None, "tp"),
    )
    out_specs = P("sp", "tp")
    return jax.shard_map(
        per_device, mesh=mesh, in_specs=in_specs, out_specs=out_specs, check_vma=False
    )
```
